32 devices in a mesh: grp: 2 (over y), fs: 4 (over z), tp: 4 (over x, core).
Axes of the slice: x: 2, y: 2, z: 4, core: 2. Of those that a mesh axis runs over, the one named last changes fastest.
Arguments:
- tokens: bfloat16 [2048, 2048], P(('grp', 'fs')), parts along dimension 0, may hold values from -6 to 6
- ffn_pre_gain: bfloat16 [2048], replicated, may hold values from 0.099609375 to 1.8984375
- gate_weight: bfloat16 [2048, 5632], P('fs', 'tp'), may hold values from -0.125 to 0.125
- up_weight: bfloat16 [2048, 5632], P('fs', 'tp'), may hold values from -0.125 to 0.125
- down_weight: bfloat16 [5632, 2048], P('tp', 'fs'), may hold values from -0.078125 to 0.078125
- ffn_post_gain: bfloat16 [2048], replicated, may hold values from 0.099609375 to 1.8984375
- mix_pre_gain: bfloat16 [2048], replicated, may hold values from 0.099609375 to 1.8984375
- mix_u_weight: bfloat16 [2048, 2048], P('fs', 'tp'), may hold values from -0.125 to 0.125
- mix_v_weight: bfloat16 [2048, 2048], P('fs', 'tp'), may hold values from -0.125 to 0.125
- spatial_gain: bfloat16 [2048], P('tp'), may hold values from 0.099609375 to 1.8984375
- spatial_weight: bfloat16 [16, 128, 128], P('tp'), may hold values from -0.5 to 0.5
- spatial_bias: bfloat16 [16, 128], P('tp'), may hold values from 0.099609375 to 1.8984375
- mix_out_weight: bfloat16 [2048, 2048], P('tp', 'fs'), may hold values from -0.125 to 0.125
- mix_post_gain: bfloat16 [2048], replicated, may hold values from 0.099609375 to 1.8984375
- late_pre_gain: bfloat16 [2048], replicated, may hold values from 0.099609375 to 1.8984375
- late_post_gain: bfloat16 [2048], replicated, may hold values from 0.099609375 to 1.8984375
Outputs:
- result: bfloat16 [2048, 2048], P(('grp', 'fs')), parts along dimension 0
The draws below stay inside these ranges and needn't reach their ends.
There are 2 independent parts, one for each index of `grp`. The reference program is written for one: setup_inputs(seed, part) draws one part's arguments, and reference() takes and returns one part's arrays. A program takes and returns all parts, laid end to end along the dimension named above; an argument that names none is the same for every part. Nothing has to cross between parts.
All inputs are finite; a program needn't handle non-finite values.
Results may differ from the reference program's by a relative error of at most 0.019.
Values may be sent and summed in bfloat16 or wider, within the bound.
No kernel may reach another device: no remote copies, remote signals or barrier semaphores. Data moves between devices by JAX's collectives and lax.ppermute only.
A program may use at most 128 MiB of HBM per device.

```python
import jax
import jax.numpy as jnp
from jax import lax

D = 2048
FF = 5632
MIX_WIDTH = 2048
GROUP_WIDTH = 128
BLOCK = 128
GROUPS = 16
TOKENS = 1024
N_TP = 4


def block_scale(stream_key, extent, split, smallest, top_value):
    def one(dim, shards_of):
        steps = jax.random.uniform(jax.random.fold_in(jax.random.fold_in(stream_key, 6), dim), (shards_of,), jnp.float32, smallest / len(split), top_value / len(split))
        return jnp.repeat(jnp.exp(steps), extent[dim] // shards_of).reshape((-1,) + (1,) * (len(extent) - dim - 1))

    loudness = one(*split[0])
    for cut in split[1:]:
        loudness = loudness * one(*cut)
    return loudness


def noise(own_key, dims, scale, reach, cuts=(), kind=jnp.bfloat16):
    entries = jax.random.normal(own_key, dims, jnp.float32) * scale
    if len(cuts) > 0:
        entries = block_scale(own_key, dims, cuts, -0.22, 0.18) * entries
    return jnp.clip(entries, min=-reach, max=reach).astype(kind)


def setup_inputs(seed: int = 0, part: int = 0) -> dict:
    seeds = jax.random.split(jax.random.key(seed), 17)
    own_keys = jax.random.split(jax.random.fold_in(seeds[16], part), 17)
    return {
        "tokens": noise(own_keys[0], (TOKENS, D), 1.0, 6.0, ((0, 4),)),
        "ffn_pre_gain": jnp.clip(1.0 + 0.18 * jax.random.normal(seeds[1], (D,), jnp.float32), 0.099609375, 1.8984375).astype(jnp.bfloat16),
        "gate_weight": noise(seeds[2], (D, FF), D ** -0.5, 0.125, ((0, 4), (1, 4))),
        "up_weight": noise(seeds[3], (D, FF), D ** -0.5, 0.125, ((0, 4), (1, 4))),
        "down_weight": noise(seeds[4], (FF, D), FF ** -0.5, 0.078125, ((0, 4), (1, 4))),
        "ffn_post_gain": jnp.clip(1.0 + 0.18 * jax.random.normal(seeds[5], (D,), jnp.float32), 0.099609375, 1.8984375).astype(jnp.bfloat16),
        "mix_pre_gain": jnp.clip(1.0 + 0.18 * jax.random.normal(seeds[6], (D,), jnp.float32), 0.099609375, 1.8984375).astype(jnp.bfloat16),
        "mix_u_weight": noise(seeds[7], (D, MIX_WIDTH), D ** -0.5, 0.125, ((0, 4), (1, 4))),
        "mix_v_weight": noise(seeds[8], (D, MIX_WIDTH), D ** -0.5, 0.125, ((0, 4), (1, 4))),
        "spatial_gain": jnp.clip(1.0 + 0.18 * jax.random.normal(seeds[9], (MIX_WIDTH,), jnp.float32), 0.099609375, 1.8984375).astype(jnp.bfloat16),
        "spatial_weight": noise(seeds[10], (GROUPS, BLOCK, BLOCK), BLOCK ** -0.5, 0.5, ((0, 4),)),
        "spatial_bias": jnp.clip(1.0 + 0.18 * jax.random.normal(seeds[11], (GROUPS, BLOCK), jnp.float32), 0.099609375, 1.8984375).astype(jnp.bfloat16),
        "mix_out_weight": noise(seeds[12], (MIX_WIDTH, D), MIX_WIDTH ** -0.5, 0.125, ((0, 4), (1, 4))),
        "mix_post_gain": jnp.clip(1.0 + 0.18 * jax.random.normal(seeds[13], (D,), jnp.float32), 0.099609375, 1.8984375).astype(jnp.bfloat16),
        "late_pre_gain": jnp.clip(1.0 + 0.18 * jax.random.normal(seeds[14], (D,), jnp.float32), 0.099609375, 1.8984375).astype(jnp.bfloat16),
        "late_post_gain": jnp.clip(1.0 + 0.18 * jax.random.normal(seeds[15], (D,), jnp.float32), 0.099609375, 1.8984375).astype(jnp.bfloat16),
    }


def row_norm(values, gain):
    scale = lax.rsqrt(lax.optimization_barrier(jnp.mean(values * values, axis=-1, keepdims=True)) + 1e-06)
    return values * scale * gain.astype(jnp.float32)

def split_sum(left, right, pieces):
    width = left.shape[1] // pieces
    total = jnp.zeros((left.shape[0], right.shape[1]), jnp.float32)
    for index in range(pieces):
        partial_term = jnp.dot(left[:, index * width:(index + 1) * width], right[index * width:(index + 1) * width], preferred_element_type=jnp.float32)
        rounded = lax.optimization_barrier(partial_term.astype(jnp.bfloat16))
        total = total + rounded.astype(jnp.float32)
    return total

def feed_forward(stream, pre_gain, post_gain, gate_weight, up_weight, down_weight):
    normed = row_norm(stream.astype(jnp.float32), pre_gain).astype(jnp.bfloat16)
    gate = jnp.dot(normed, gate_weight, preferred_element_type=jnp.float32)
    upper = jnp.dot(normed, up_weight, preferred_element_type=jnp.float32)
    hidden = (jax.nn.silu(gate) * upper).astype(jnp.bfloat16)
    branch = split_sum(hidden, down_weight, N_TP)
    return (stream.astype(jnp.float32) + 0.5 * row_norm(branch, post_gain)).astype(jnp.bfloat16)

def reference(tokens, ffn_pre_gain, gate_weight, up_weight, down_weight, ffn_post_gain, mix_pre_gain, mix_u_weight, mix_v_weight, spatial_gain, spatial_weight, spatial_bias, mix_out_weight, mix_post_gain, late_pre_gain, late_post_gain):
    first = feed_forward(tokens, ffn_pre_gain, ffn_post_gain, gate_weight, up_weight, down_weight)
    normed = row_norm(first.astype(jnp.float32), mix_pre_gain).astype(jnp.bfloat16)
    gated_u = jax.nn.gelu(jnp.dot(normed, mix_u_weight, preferred_element_type=jnp.float32), approximate=False)
    gating_v = jax.nn.gelu(jnp.dot(normed, mix_v_weight, preferred_element_type=jnp.float32), approximate=False)
    count = gating_v.shape[0]
    grouped = gating_v.reshape(count, GROUPS, GROUP_WIDTH)
    centred = grouped - lax.optimization_barrier(jnp.mean(grouped, axis=-1, keepdims=True))
    vnorm = centred * lax.rsqrt(lax.optimization_barrier(jnp.mean(centred * centred, axis=-1, keepdims=True)) + 1e-05)
    vnorm = (vnorm * spatial_gain.astype(jnp.float32).reshape(GROUPS, GROUP_WIDTH)).astype(jnp.bfloat16)
    blocks = vnorm.reshape(count // BLOCK, BLOCK, GROUPS, GROUP_WIDTH).astype(jnp.float32)
    lower = jnp.tril(jnp.ones((BLOCK, BLOCK), dtype=bool))
    masked = jnp.where(lower[None], spatial_weight, jnp.zeros_like(spatial_weight)).astype(jnp.float32)
    spatial = jnp.einsum('gts,nsgc->ntgc', masked, blocks)
    spatial = spatial + spatial_bias.astype(jnp.float32).T[None, :, :, None]
    mixed = (gated_u * spatial.reshape(count, MIX_WIDTH)).astype(jnp.bfloat16)
    branch = split_sum(mixed, mix_out_weight, N_TP)
    second = (first.astype(jnp.float32) + row_norm(branch, mix_post_gain)).astype(jnp.bfloat16)
    return feed_forward(second, late_pre_gain, late_post_gain, gate_weight, up_weight, down_weight)
```

```python
import jax
import jax.numpy as jnp
from jax import lax
from jax.sharding import PartitionSpec as P

GROUP_WIDTH = 128
BLOCK = 128
CORES = 2


SEGMENTS = 4


def row_norm(values, gain):
    scale = lax.rsqrt(jnp.mean(values * values, axis=-1, keepdims=True) + 1e-06)
    return values * scale * gain.astype(jnp.float32)


def gelu(values):
    return jax.nn.gelu(values, approximate=False)


def solution(mesh):
    grp_size, fs_size, tp_size = mesh.shape["grp"], mesh.shape["fs"], mesh.shape["tp"]
    stride = fs_size // SEGMENTS
    chips = tp_size // CORES

    def hops(moves):
        return [(a * stride + i, b * stride + i) for a, b in moves for i in range(stride)]

    near_hops = hops([(0, 1), (3, 2)])
    home_hops = hops([(1, 0), (2, 3)])
    mid_hops = hops([(1, 2), (2, 1)])
    core_swap = [(i, i ^ 1) for i in range(tp_size)]

    def chip_turn(step):
        return [
            (x * CORES + c, (x + step) % chips * CORES + c) for x in range(chips) for c in range(CORES)
        ]

    def grp_turn(step):
        return [(i, (i + step) % grp_size) for i in range(grp_size)]

    def from_near(value):
        return lax.ppermute(value, "fs", near_hops)

    def from_mid(value):
        return lax.ppermute(value, "fs", mid_hops)

    def swap_core(value):
        return lax.ppermute(value, "tp", core_swap)

    def segment_gather(weight, axis):
        if stride == 1:
            return weight
        ring = [
            (s * stride + i, s * stride + (i + 1) % stride) for s in range(SEGMENTS) for i in range(stride)
        ]
        parts = [weight]
        for _ in range(stride - 1):
            parts.append(lax.ppermute(parts[-1], "fs", ring))
        place = lax.axis_index("fs") % stride
        stacked = jnp.stack(parts[::-1])
        ordered = jnp.roll(stacked, place + 1, axis=0)
        return jnp.concatenate([ordered[i] for i in range(stride)], axis=axis)

    def shards(
        tokens,
        ffn_pre_gain,
        gate_weight,
        up_weight,
        down_weight,
        ffn_post_gain,
        mix_pre_gain,
        mix_u_weight,
        mix_v_weight,
        spatial_gain,
        spatial_weight,
        spatial_bias,
        mix_out_weight,
        mix_post_gain,
        late_pre_gain,
        late_post_gain,
    ):
        count, width = tokens.shape
        segment = lax.axis_index("fs") // stride
        grp = lax.axis_index("grp")
        tp = lax.axis_index("tp")
        core = tp % CORES
        chip = tp // CORES
        is_left = segment < SEGMENTS // 2
        is_host = (segment == 1) | (segment == 2)
        block = width // SEGMENTS
        piece = block // grp_size
        half = count // CORES

        def cut(values, size):
            return [values[..., i : i + size] for i in range(0, values.shape[-1], size)]

        def turn_parts(values, sign):
            parts = cut(values, piece)
            if grp_size == 1:
                return values
            turned = values
            for g in range(1, grp_size):
                order = [parts[(i + sign * g) % grp_size] for i in range(grp_size)]
                turned = jnp.where(grp == g, jnp.concatenate(order, axis=-1), turned)
            return turned

        def to_host_order(values):
            s = cut(values, block)
            blocks = [jnp.where(is_left, s[a], s[b]) for a, b in ((1, 2), (0, 3), (2, 1), (3, 0))]
            return jnp.concatenate([turn_parts(b, 1) for b in blocks], axis=-1)

        def to_natural_order(values):
            s = [turn_parts(b, -1) for b in cut(values, block)]
            blocks = [jnp.where(is_left, s[a], s[b]) for a, b in ((1, 3), (0, 2), (2, 0), (3, 1))]
            return jnp.concatenate(blocks, axis=-1)

        def own_parts(weight, axis):
            weight = segment_gather(weight, axis)
            return [
                lax.dynamic_slice_in_dim(weight, (grp + r) % grp_size * piece, piece, axis=axis)
                for r in range(grp_size)
            ]

        def share_grp(part):
            return [part] + [
                lax.ppermute(part, "grp", grp_turn(-r)) for r in range(1, grp_size)
            ]

        def gather_parts(weight, axis):
            own = own_parts(weight, axis)
            near = [from_near(part) for part in own]
            mid = share_grp(from_mid(own[0]))
            far = share_grp(from_mid(near[0]))
            return own + near + mid + far

        share = count // tp_size
        sent = from_near(lax.dynamic_slice_in_dim(tokens, tp * share, share, axis=0))
        slots = [sent] + [lax.ppermute(sent, "tp", chip_turn(-s)) for s in range(1, chips)]
        slots = slots + [swap_core(slot) for slot in slots]

        def pick(index):
            wanted_chip, wanted_core = index // CORES, index % CORES
            turn = (wanted_chip - chip) % chips
            value = slots[0]
            for c in range(CORES):
                for s in range(chips):
                    if c + s:
                        hit = (turn == s) & ((wanted_core != core) == (c == 1))
                        value = jnp.where(hit, slots[c * chips + s], value)
            return value

        guest = jnp.concatenate([pick(i) for i in range(tp_size)], axis=0)

        gains = jnp.stack(
            [ffn_pre_gain, ffn_post_gain, mix_pre_gain, mix_post_gain, late_pre_gain, late_post_gain]
        )
        gains = to_host_order(gains)

        gate_parts = gather_parts(gate_weight, 0)
        up_parts = gather_parts(up_weight, 0)
        down_parts = gather_parts(down_weight, 1)
        u_parts = gather_parts(mix_u_weight, 0)
        v_parts = gather_parts(mix_v_weight, 0)
        out_parts = gather_parts(mix_out_weight, 1)
        gate_full = jnp.concatenate(gate_parts, axis=0)
        up_full = jnp.concatenate(up_parts, axis=0)
        down_full = jnp.concatenate(down_parts, axis=1)
        u_full = jnp.concatenate(u_parts, axis=0)
        v_full = jnp.concatenate(v_parts, axis=0)
        out_full = jnp.concatenate(out_parts, axis=1)

        def my_half(values):
            return lax.dynamic_slice_in_dim(values, core * half, half, axis=0)

        def other_half(values):
            return lax.dynamic_slice_in_dim(values, (1 - core) * half, half, axis=0)

        def join_halves(mine):
            other = swap_core(mine)
            return jnp.where(
                core == 0, jnp.concatenate([mine, other], axis=0), jnp.concatenate([other, mine], axis=0)
            )

        def reduce_half(terms):
            terms = terms.astype(jnp.bfloat16)
            both = my_half(terms).astype(jnp.float32) + swap_core(other_half(terms)).astype(jnp.float32)
            both = both.astype(jnp.bfloat16)
            slices = [both] + [lax.ppermute(both, "tp", chip_turn(-s)) for s in range(1, chips)]
            if chips > 2:
                ordered = jnp.roll(jnp.stack(slices), chip, axis=0)
                slices = [ordered[i] for i in range(chips)]
            total = slices[0].astype(jnp.float32)
            for term in slices[1:]:
                total = total + term.astype(jnp.float32)
            return total

        def add_branch(stream, total, gain, factor):
            return (stream.astype(jnp.float32) + factor * row_norm(total, gain)).astype(jnp.bfloat16)

        def normed_of(stream, gain):
            return row_norm(stream.astype(jnp.float32), gain).astype(jnp.bfloat16)

        def hidden_of(normed):
            gate = jnp.dot(normed, gate_full, preferred_element_type=jnp.float32)
            upper = jnp.dot(normed, up_full, preferred_element_type=jnp.float32)
            return (jax.nn.silu(gate) * upper).astype(jnp.bfloat16)

        groups = mix_u_weight.shape[1] // GROUP_WIDTH
        lower = jnp.tril(jnp.ones((BLOCK, BLOCK), dtype=bool))
        masked = jnp.where(lower[None], spatial_weight, jnp.zeros_like(spatial_weight))

        def mix(normed):
            gated_u = gelu(jnp.dot(normed, u_full, preferred_element_type=jnp.float32))
            gating_v = gelu(jnp.dot(normed, v_full, preferred_element_type=jnp.float32))
            grouped = gating_v.reshape(count, groups, GROUP_WIDTH)
            centred = grouped - jnp.mean(grouped, axis=-1, keepdims=True)
            vnorm = centred * lax.rsqrt(jnp.mean(centred * centred, axis=-1, keepdims=True) + 1e-05)
            vnorm = (vnorm * spatial_gain.astype(jnp.float32).reshape(groups, GROUP_WIDTH)).astype(
                jnp.bfloat16
            )
            blocks = vnorm.reshape(count // BLOCK, BLOCK, groups, GROUP_WIDTH)
            spatial = jnp.einsum("gts,nsgc->ntgc", masked, blocks, preferred_element_type=jnp.float32)
            spatial = spatial + spatial_bias.astype(jnp.float32).T[None, :, :, None]
            mixed = (gated_u * spatial.reshape(count, groups * GROUP_WIDTH)).astype(jnp.bfloat16)
            return jnp.dot(mixed, out_full, preferred_element_type=jnp.float32)

        streams = to_host_order(jnp.concatenate([guest, tokens], axis=0))
        hidden = hidden_of(normed_of(streams, gains[0]))
        terms = jnp.dot(hidden, down_full, preferred_element_type=jnp.float32)
        results = []
        for index in range(2):
            rows = slice(index * count, (index + 1) * count)
            first = add_branch(my_half(streams[rows]), reduce_half(terms[rows]), gains[1], 0.5)
            mixed = mix(join_halves(normed_of(first, gains[2])))
            second = add_branch(first, reduce_half(mixed), gains[3], 1.0)
            late = hidden_of(join_halves(normed_of(second, gains[4])))
            late = jnp.dot(late, down_full, preferred_element_type=jnp.float32)
            result = add_branch(second, reduce_half(late), gains[5], 0.5)
            results.append(to_natural_order(result))
        sent_home = lax.ppermute(results[0], "fs", home_hops)
        return join_halves(jnp.where(is_host, results[1], sent_home))

    in_specs = (
        P(("grp", "fs"), None),
        P(),
        P("fs", "tp"),
        P("fs", "tp"),
        P("tp", "fs"),
        P(),
        P(),
        P("fs", "tp"),
        P("fs", "tp"),
        P("tp"),
        P("tp", None, None),
        P("tp", None),
        P("tp", "fs"),
        P(),
        P(),
        P(),
    )
    out_specs = P(("grp", "fs"), None)
    return jax.shard_map(shards, mesh=mesh, in_specs=in_specs, out_specs=out_specs, check_vma=False)
```
